32 devices in a mesh: kv: 16 (over z, x, core), tp: 2 (over y).
Axes of the slice: x: 2, y: 2, z: 4, core: 2. Of those that a mesh axis runs over, the one named last changes fastest.
Arguments:
- queries: bfloat16 [2048, 4096], P('kv', 'tp'), may hold values from -6 to 6
- keys: bfloat16 [2048, 512], P('kv', 'tp'), may hold values from -6 to 6
- values: bfloat16 [2048, 512], P('kv', 'tp'), may hold values from -6 to 6
- logsum: float32 [2048, 32], P('kv', 'tp'), may hold values from 2 to 6
- out_grad: bfloat16 [2048, 4096], P('kv', 'tp'), may hold values from -6 to 6
- normed_input: bfloat16 [2048, 4096], P('kv', 'tp'), may hold values from -6 to 6
- chosen: int32 [32, 16], P('kv'), may hold values from 0 to 63, as said below
Outputs:
- query_grad: float32 [2048, 4096], P('kv', 'tp')
- key_grad: float32 [2048, 512], P('kv', 'tp')
- value_grad: float32 [2048, 512], P('kv', 'tp')
- value_weight_grad: float32 [4096, 512], P('kv', 'tp')
The draws below stay inside these ranges and needn't reach their ends.
Inputs may be any that keep to these rules, and one draw needn't show every extreme that they name: `chosen`: each row r names 16 distinct key blocks, among them block 0 and the blocks r * 2 to r * 2 + 64 / 32 - 1 that hold the query block's own positions. The rows of one device (aligned runs of 2 rows) name at most one block of any other device's 128 / 32 blocks. Blocks after the query block may be named; their keys are masked.
All inputs are finite; a program needn't handle non-finite values.
Results may differ from the reference program's by a relative error of at most 0.008.
Values may be sent and summed in bfloat16 or wider, within the bound.
A program may use at most 64 MiB of HBM per device.

```python
import jax
import jax.numpy as jnp
from jax import lax

D = 4096
HEADS = 32
KV_HEADS = 4
HD = 128
TOK_DEV = 128
QB = 64
KB = 32
NSEL = 16
TOKENS = 2048


def draw_chosen(key, part):
    kblock_count = TOK_DEV // KB
    qblock_count = TOK_DEV // QB
    devices = TOKENS // TOK_DEV
    row_count = TOKENS // QB
    diag = QB // KB
    ncand = devices + kblock_count
    key_pick = jax.random.fold_in(key, 11)
    key_pop = jax.random.fold_in(key, 12)
    key_far = jax.random.fold_in(key, 13)
    key_own = jax.random.fold_in(key, 14)
    owners = jnp.arange(devices, dtype=jnp.int32)
    pick = jax.random.randint(key_pick, (devices, devices), 0, kblock_count)
    pick = jnp.where(owners[None, :] == 0, 0, pick)
    popular = jax.random.randint(key_pop, (devices,), 0, 8)
    rows = jnp.arange(row_count, dtype=jnp.int32)
    device_of = rows // qblock_count
    first = rows * diag
    remote_blk = owners[None, :] * kblock_count + pick[device_of]
    own_blk = device_of[:, None] * kblock_count + jnp.arange(kblock_count, dtype=jnp.int32)[None, :]
    cand = jnp.concatenate([remote_blk, own_blk], axis=1)
    cand_owner = cand // kblock_count
    slot_owner = jnp.concatenate([owners, jnp.full((kblock_count,), -1, jnp.int32)])
    is_diag = (cand >= first[:, None]) & (cand < first[:, None] + diag)
    invalid = (slot_owner[None, :] == device_of[:, None]) | is_diag
    forced = (cand == 0) | (cand_owner == device_of[:, None] - 1) | (cand_owner == device_of[:, None] - devices // 2)
    causal = cand < first[:, None]
    far_noise = jax.random.randint(key_far, (row_count, devices), 0, 32) + popular[None, :]
    own_noise = jax.random.randint(key_own, (row_count, kblock_count), 0, 32)
    noise = jnp.concatenate([far_noise, own_noise], axis=1)
    tier = jnp.where(forced, 3, jnp.where(causal, 2, 1))
    index = jnp.arange(ncand, dtype=jnp.int32)[None, :]
    score = jnp.where(invalid, 0, tier * 64 + noise) * ncand + (ncand - 1 - index)
    _, top = lax.top_k(score, NSEL - diag)
    picked = jnp.take_along_axis(cand, top, axis=1)
    diag_ids = first[:, None] + jnp.arange(diag, dtype=jnp.int32)[None, :]
    return jnp.concatenate([diag_ids, picked], axis=1).astype(jnp.int32)


def block_levels(stream_key, extent, split, least, high):
    loudness, own = 1.0, jax.random.fold_in(stream_key, 6)
    for position, blocks in split:
        steps = jnp.exp(jax.random.uniform(jax.random.fold_in(own, position), (blocks,), jnp.float32, least / len(split), high / len(split)))
        loudness = loudness * jnp.repeat(steps, extent[position] // blocks).reshape([-1 if axis == position else 1 for axis in range(len(extent))])
    return loudness


def bell_draw(stream_key, dims, width, limit, shards=(), kind=jnp.bfloat16):
    gain = block_levels(stream_key, dims, shards, -0.22, 0.18) if shards else 1.0
    drawn = jax.random.normal(stream_key, dims, jnp.float32) * width * gain
    return jnp.minimum(jnp.maximum(drawn, -limit), limit).astype(kind)


def setup_inputs(seed: int = 0) -> dict:
    streams_of = jax.random.split(jax.random.key(seed), 8)
    return {
        "queries": bell_draw(streams_of[0], (TOKENS, HEADS * HD), 1.0, 6.0, ((0, 16), (1, 2))),
        "keys": bell_draw(streams_of[1], (TOKENS, KV_HEADS * HD), 1.0, 6.0, ((0, 16), (1, 2))),
        "values": bell_draw(streams_of[2], (TOKENS, KV_HEADS * HD), 1.0, 6.0, ((0, 16), (1, 2))),
        "logsum": jnp.clip(2.0 + 4.0 * jax.random.uniform(streams_of[3], (TOKENS, HEADS), jnp.float32) ** block_levels(streams_of[3], (TOKENS, HEADS), ((0, 16), (1, 2)), -0.2, 0.2), 2.0, 6.0),
        "out_grad": bell_draw(streams_of[4], (TOKENS, HEADS * HD), 1.0, 6.0, ((0, 16), (1, 2))),
        "normed_input": bell_draw(streams_of[5], (TOKENS, D), 1.0, 6.0, ((0, 16), (1, 2))),
        "chosen": draw_chosen(jax.random.fold_in(streams_of[7], 71), 0),
    }


def reference(queries, keys, values, logsum, out_grad, normed_input, chosen):
    group = HEADS // KV_HEADS
    kv_cols = KV_HEADS * HD
    scale = HD ** -0.5
    blocks = TOKENS // KB
    key_blocks = keys.reshape(blocks, KB, KV_HEADS, HD)
    value_blocks = values.reshape(blocks, KB, KV_HEADS, HD)
    offsets = jnp.arange(KB, dtype=jnp.int32)
    rows_in = jnp.arange(QB, dtype=jnp.int32)

    def step(carry, index):
        key_acc, value_acc = carry
        ids = chosen[index]
        start = index * QB
        query_rows = lax.dynamic_slice_in_dim(queries, start, QB, 0).reshape(QB, KV_HEADS, group, HD).astype(jnp.float32)
        dout = lax.dynamic_slice_in_dim(out_grad, start, QB, 0).reshape(QB, KV_HEADS, group, HD).astype(jnp.float32)
        lse = lax.dynamic_slice_in_dim(logsum, start, QB, 0).reshape(QB, KV_HEADS, group)
        sel_keys = key_blocks[ids].reshape(NSEL * KB, KV_HEADS, HD).astype(jnp.float32)
        sel_values = value_blocks[ids].reshape(NSEL * KB, KV_HEADS, HD).astype(jnp.float32)
        scores = jnp.einsum("qngd,jnd->qngj", query_rows, sel_keys) * scale
        qpos = start + rows_in
        kpos = (ids[:, None] * KB + offsets[None, :]).reshape(NSEL * KB)
        valid = (kpos[None, :] <= qpos[:, None])[:, None, None, :]
        prob = jnp.where(valid, jnp.exp(scores - lse[..., None]), 0.0)
        dprob = jnp.einsum("qngd,jnd->qngj", dout, sel_values)
        delta = jnp.sum(prob * dprob, axis=-1, keepdims=True)
        dscore = lax.optimization_barrier((prob * (dprob - delta)).astype(jnp.bfloat16)).astype(jnp.float32)
        prob_low = lax.optimization_barrier(prob.astype(jnp.bfloat16)).astype(jnp.float32)
        query_part = jnp.einsum("qngj,jnd->qngd", dscore, sel_keys) * scale
        key_part = jnp.einsum("qngj,qngd->jnd", dscore, query_rows) * scale
        value_part = jnp.einsum("qngj,qngd->jnd", prob_low, dout)
        key_acc = key_acc.at[ids].add(key_part.reshape(NSEL, KB * kv_cols))
        value_acc = value_acc.at[ids].add(value_part.reshape(NSEL, KB * kv_cols))
        return (key_acc, value_acc), query_part.reshape(QB, HEADS * HD)

    zeros = jnp.zeros((blocks, KB * kv_cols), jnp.float32)
    (key_acc, value_acc), query_rows_all = lax.scan(step, (zeros, zeros), jnp.arange(TOKENS // QB, dtype=jnp.int32))
    query_grad = query_rows_all.reshape(TOKENS, HEADS * HD)
    key_grad = key_acc.reshape(TOKENS, kv_cols)
    value_grad = value_acc.reshape(TOKENS, kv_cols)
    value_low = value_grad.astype(jnp.bfloat16)
    weight_grad = jnp.dot(normed_input.astype(jnp.float32).T, value_low.astype(jnp.float32))
    return query_grad, key_grad, value_grad, weight_grad
```

```python
import functools

import jax
import jax.numpy as jnp
from jax import lax
from jax.experimental import pallas as pl
from jax.experimental.pallas import tpu as pltpu
from jax.sharding import PartitionSpec as P

HD = 128
QB = 64
KB = 32
NSEL = 16

MESH = pl.DeviceIdType.MESH
F32 = jnp.float32
BF16 = jnp.bfloat16


def remote(src, dst, send_sem, recv_sem, device_id):
    return pltpu.make_async_remote_copy(
        src_ref=src,
        dst_ref=dst,
        send_sem=send_sem,
        recv_sem=recv_sem,
        device_id=device_id,
        device_id_type=MESH,
    )


class Gather:
    def __init__(self, pool, send_z, send_x, send_c, recv, me, n, xs, upward):
        self.pool, self.recv = pool, recv
        self.send_z, self.send_x, self.send_c = send_z, send_x, send_c
        self.me, self.n, self.xs = me, n, xs
        self.row = 2 * xs
        self.zs = n // self.row
        self.z = me // self.row
        self.r = me % self.row
        self.x = self.r // 2
        self.c = self.r % 2
        self.sends = self.zs - 1 - self.z if upward else self.zs - 1
        self.planes = self.z + 1 if upward else self.zs

    def copy(self, slot, send_sem, dest):
        return remote(
            self.pool.at[slot], self.pool.at[slot], send_sem, self.recv.at[slot], {"kv": dest}
        )

    def plane(self, k):
        return (self.z - k + self.zs) % self.zs

    def along_z(self, k):
        dest = ((self.z + k) % self.zs) * self.row + self.r
        return self.copy(self.me, self.send_z.at[k], dest)

    def along_x(self, k, d):
        slot = self.plane(k) * self.row + self.r
        dest = self.z * self.row + ((self.x + d) % self.xs) * 2 + self.c
        return self.copy(slot, self.send_x.at[k, d], dest)

    def across(self, k, d):
        slot = self.plane(k) * self.row + ((self.x + d) % self.xs) * 2 + self.c
        dest = self.z * self.row + self.x * 2 + (1 - self.c)
        return self.copy(slot, self.send_c.at[k, d], dest)

    def wait_slot(self, slot):
        self.copy(slot, self.send_z.at[0], (self.me + 1) % self.n).wait_recv()

    def start(self):
        def body(k, _):
            self.along_z(k).start()
            return 0

        lax.fori_loop(1, self.sends + 1, body, 0)

    def relay(self):
        def step(k, first):
            slot = self.plane(k) * self.row + self.r
            if not first:
                self.wait_slot(slot)
            for d in range(1, self.xs):
                self.along_x(k, d).start()
            self.across(k, 0).start()

        def cross(k):
            for d in range(1, self.xs):
                slot = self.plane(k) * self.row + ((self.x + d) % self.xs) * 2 + self.c
                self.wait_slot(slot)
                self.across(k, d).start()

        step(0, True)

        def body(k, _):
            step(k, False)
            cross(k - 1)
            return 0

        lax.fori_loop(1, self.planes, body, 0)
        cross(self.planes - 1)

    def finish(self):
        def body(k, _):
            for d in range(self.xs):
                self.wait_slot(
                    self.plane(k) * self.row + ((self.x + d) % self.xs) * 2 + (1 - self.c)
                )
            return 0

        lax.fori_loop(0, self.planes, body, 0)

    def drain(self):
        def zbody(k, _):
            self.along_z(k).wait_send()
            return 0

        lax.fori_loop(1, self.sends + 1, zbody, 0)

        def body(k, _):
            for d in range(1, self.xs):
                self.along_x(k, d).wait_send()
            for d in range(self.xs):
                self.across(k, d).wait_send()
            return 0

        lax.fori_loop(0, self.planes, body, 0)


def dot(a, b, dims):
    return lax.dot_general(a, b, (dims, ((), ())), preferred_element_type=F32)


def kernel(
    n,
    tp,
    chosen_s,
    chosen_v,
    queries,
    keys,
    values,
    lse,
    out_grad,
    normed_t,
    query_grad,
    key_grad,
    value_grad,
    weight_grad,
    pool,
    low_pool,
    norm_pool,
    chosen_all,
    hit,
    sel,
    s_buf,
    d_buf,
    p_low,
    ds_low,
    part,
    back,
    got,
    table,
    local_sem,
    kv_z,
    kv_x,
    kv_c,
    kv_recv,
    lo_z,
    lo_x,
    lo_c,
    lo_recv,
    n_send,
    n_recv,
    c_send,
    c_recv,
    g_send,
    g_recv,
):
    me = lax.axis_index("kv")
    col = lax.axis_index("tp")
    kblocks = keys.shape[0]
    tok = kblocks * KB
    qblocks = tok // QB
    kv_cols = keys.shape[2]
    kv_heads = kv_cols // HD
    group = queries.shape[1] // kv_cols
    rows = normed_t.shape[0] * tp // n
    per = n // tp
    scale = HD ** (-0.5)
    entries = qblocks * NSEL

    own = [
        pltpu.make_async_copy(keys, pool.at[me, 0], local_sem.at[0]),
        pltpu.make_async_copy(values, pool.at[me, 1], local_sem.at[1]),
    ]
    for c in own:
        c.start()

    barrier = pltpu.get_barrier_semaphore()

    def greet(i, _):
        for t in range(tp):
            pl.semaphore_signal(
                barrier, inc=1, device_id={"kv": i, "tp": t}, device_id_type=MESH
            )
        return 0

    lax.fori_loop(0, n, greet, 0)
    for c in own:
        c.wait()
    pl.semaphore_wait(barrier, n * tp)

    kv = Gather(pool, kv_z, kv_x, kv_c, kv_recv, me, n, tp, True)
    kv.start()

    def chosen_copy(i):
        return remote(
            chosen_v, chosen_all.at[me], c_send.at[i], c_recv.at[me], {"kv": i}
        )

    def ask(i, _):
        chosen_copy(i).start()
        return 0

    lax.fori_loop(0, me, ask, 0)
    kv.relay()

    def norm_copy(k, t):
        dest = col * per + k
        return remote(
            normed_t.at[pl.ds(pl.multiple_of(k * rows, rows), rows)],
            norm_pool.at[me],
            n_send.at[k, t],
            n_recv.at[me],
            {"kv": dest, "tp": t},
        )

    def norm_local(k):
        return pltpu.make_async_copy(
            normed_t.at[pl.ds(pl.multiple_of(k * rows, rows), rows)],
            norm_pool.at[me],
            n_recv.at[me],
        )

    def norm_each(act, act_local):
        def body(k0, _):
            k = (k0 + me) % per
            for t in range(tp):
                self_dest = (col * per + k == me) & (col == t)

                @pl.when(self_dest)
                def _():
                    act_local(k)

                @pl.when(jnp.logical_not(self_dest))
                def _():
                    act(k, t)

            return 0

        lax.fori_loop(0, per, body, 0)

    norm_each(lambda k, t: norm_copy(k, t).start(), lambda k: norm_local(k).start())

    def look(i, _):
        for b in range(qblocks):
            found = jnp.int32(entries)
            for e in range(NSEL):
                found = jnp.where(chosen_s[b, e] // kblocks == i, b * NSEL + e, found)
            table[b, i] = found
        return 0

    lax.fori_loop(0, me, look, 0)
    for w in range(kblocks):
        for b in range(qblocks):
            found = jnp.int32(entries)
            for e in range(NSEL):
                found = jnp.where(chosen_s[b, e] == me * kblocks + w, b * NSEL + e, found)
            table[b, n + w] = found
    part[:, entries] = jnp.zeros_like(part[:, entries])

    kv.finish()
    plane_end = (kv.z + 1) * kv.row * kblocks
    span = NSEL * KB
    width = group * QB
    key_iota = lax.broadcasted_iota(jnp.int32, (KB, width), 0)
    row_iota = lax.broadcasted_iota(jnp.int32, (KB, width), 1) % QB
    for b in range(qblocks):
        for e in range(NSEL):
            block = chosen_s[b, e]
            block = jnp.where(block < plane_end, block, 0)
            for a in range(2):
                sel[a, e * KB : (e + 1) * KB, :] = pool[block // kblocks, a, block % kblocks]
        for g in range(kv_heads):
            lanes = slice(g * HD, (g + 1) * HD)

            def stack(ref):
                return jnp.concatenate(
                    [
                        ref[b * QB : (b + 1) * QB, (g * group + h) * HD : (g * group + h + 1) * HD]
                        for h in range(group)
                    ],
                    axis=0,
                )

            q = stack(queries)
            do = stack(out_grad)
            k_sel = sel[0, :, lanes]
            s_buf[...] = dot(k_sel, q, ((1,), (1,)))
            d_buf[...] = dot(sel[1, :, lanes], do, ((1,), (1,)))
            log = lse[b, g]
            delta = jnp.zeros((8, width), F32)
            for e in range(NSEL):
                at = slice(e * KB, (e + 1) * KB)
                limit = (me * tok + b * QB) - chosen_s[b, e] * KB
                valid = key_iota - row_iota <= limit
                p = jnp.where(valid, jnp.exp(s_buf[at, :] * scale - log), 0.0)
                s_buf[at, :] = p
                p_low[at, :] = p.astype(BF16)
                pd = p * d_buf[at, :]
                delta = delta + jnp.sum(pd.reshape(KB // 8, 8, width), axis=0)
            delta = jnp.sum(delta, axis=0, keepdims=True)
            for e in range(NSEL):
                at = slice(e * KB, (e + 1) * KB)
                ds_low[at, :] = (s_buf[at, :] * (d_buf[at, :] - delta)).astype(BF16)
            ds = ds_low[...]
            here = slice(b * NSEL, (b + 1) * NSEL)
            part[0, here, :, lanes] = (dot(ds, q, ((1,), (0,))) * scale).reshape(NSEL, KB, HD)
            part[1, here, :, lanes] = dot(p_low[...], do, ((1,), (0,))).reshape(NSEL, KB, HD)
            dq = dot(ds, k_sel, ((0,), (0,))) * scale
            for h in range(group):
                query_grad[
                    b * QB : (b + 1) * QB, (g * group + h) * HD : (g * group + h + 1) * HD
                ] = dq[h * QB : (h + 1) * QB]

    def back_copy(i):
        return remote(back.at[i], got.at[me], g_send.at[i], g_recv.at[me], {"kv": i})

    def send_back(i, _):
        for a in range(2):
            total = part[a, table[0, i]]
            for b in range(1, qblocks):
                total = total + part[a, table[b, i]]
            back[i, a] = total.astype(BF16)
        back_copy(i).start()
        return 0

    lax.fori_loop(0, me, send_back, 0)

    for w in range(kblocks):
        for a, out in ((0, key_grad), (1, value_grad)):
            total = part[a, table[0, n + w]]
            for b in range(1, qblocks):
                total = total + part[a, table[b, n + w]]
            out[w] = total

    def heard(j, _):
        remote(
            chosen_v, chosen_all.at[j], c_send.at[0], c_recv.at[j], {"kv": (me + 1) % n}
        ).wait_recv()
        for w in range(kblocks):
            named = jnp.where(chosen_all[j] == me * kblocks + w, 1.0, 0.0)
            named = jnp.max(jnp.max(named, axis=1, keepdims=True), axis=0, keepdims=True)
            hit[j, w] = jnp.broadcast_to(named, (8, kv_cols))
        return 0

    lax.fori_loop(me + 1, n, heard, 0)

    def add_back(j, _):
        remote(
            back.at[0], got.at[j], g_send.at[0], g_recv.at[j], {"kv": (me + 1) % n}
        ).wait_recv()
        terms = [got[j, a].astype(F32) for a in range(2)]
        for w in range(kblocks):
            mask = jnp.concatenate([hit[j, w]] * (KB // 8), axis=0)
            for a, out in ((0, key_grad), (1, value_grad)):
                out[w] += mask * terms[a]
        return 0

    lax.fori_loop(me + 1, n, add_back, 0)

    low_pool[me] = value_grad[...].reshape(tok, kv_cols).astype(BF16)
    low = Gather(low_pool, lo_z, lo_x, lo_c, lo_recv, me, n, tp, False)
    low.start()
    low.relay()

    def norm_wait(j, _):
        pltpu.make_async_copy(norm_pool.at[j], norm_pool.at[j], n_recv.at[j]).wait()
        return 0

    lax.fori_loop(0, n, norm_wait, 0)
    low.finish()

    row = kv.row

    def product(z):
        a = jnp.concatenate([norm_pool[z * row + i] for i in range(row)], axis=1)
        v = jnp.concatenate([low_pool[z * row + i] for i in range(row)], axis=0)
        return dot(a, v, ((1,), (0,)))

    weight_grad[...] = product(0)

    def weigh(z, _):
        weight_grad[...] += product(z)
        return 0

    lax.fori_loop(1, kv.zs, weigh, 0)

    kv.drain()
    low.drain()

    def drain_small(i, _):
        chosen_copy(i).wait_send()
        back_copy(i).wait_send()
        return 0

    lax.fori_loop(0, me, drain_small, 0)
    norm_each(lambda k, t: norm_copy(k, t).wait_send(), lambda k: None)


def local(n, tp, queries, keys, values, logsum, out_grad, normed_input, chosen):
    tok, kv_cols = keys.shape
    kv_heads = kv_cols // HD
    group = queries.shape[1] // kv_cols
    kblocks = tok // KB
    qblocks = tok // QB
    rows = normed_input.shape[1] * tp // n
    zs = n // (2 * tp)
    entries = qblocks * NSEL
    span = NSEL * KB
    width = group * QB
    lse = (
        logsum.reshape(qblocks, QB, kv_heads, group)
        .transpose(0, 2, 3, 1)
        .reshape(qblocks, kv_heads, 1, width)
    )
    vmem = pl.BlockSpec(memory_space=pltpu.VMEM)
    dma = pltpu.SemaphoreType.DMA
    outs = pl.pallas_call(
        functools.partial(kernel, n, tp),
        out_shape=(
            jax.ShapeDtypeStruct((tok, queries.shape[1]), F32),
            jax.ShapeDtypeStruct((kblocks, KB, kv_cols), F32),
            jax.ShapeDtypeStruct((kblocks, KB, kv_cols), F32),
            jax.ShapeDtypeStruct((rows, kv_cols), F32),
        ),
        in_specs=[pl.BlockSpec(memory_space=pltpu.SMEM)] + [vmem] * 7,
        out_specs=(vmem,) * 4,
        scratch_shapes=[
            pltpu.VMEM((n, 2, kblocks, KB, kv_cols), BF16),
            pltpu.VMEM((n, tok, kv_cols), BF16),
            pltpu.VMEM((n, rows, tok), BF16),
            pltpu.VMEM((n, qblocks, NSEL), jnp.int32),
            pltpu.VMEM((n, kblocks, 8, kv_cols), F32),
            pltpu.VMEM((2, span, kv_cols), BF16),
            pltpu.VMEM((span, width), F32),
            pltpu.VMEM((span, width), F32),
            pltpu.VMEM((span, width), BF16),
            pltpu.VMEM((span, width), BF16),
            pltpu.VMEM((2, entries + 1, KB, kv_cols), F32),
            pltpu.VMEM((n, 2, KB, kv_cols), BF16),
            pltpu.VMEM((n, 2, KB, kv_cols), BF16),
            pltpu.SMEM((qblocks, n + kblocks), jnp.int32),
            dma((2,)),
            dma((zs,)),
            dma((zs, tp)),
            dma((zs, tp)),
            dma((n,)),
            dma((zs,)),
            dma((zs, tp)),
            dma((zs, tp)),
            dma((n,)),
            dma((n // tp, tp)),
            dma((n,)),
            dma((n,)),
            dma((n,)),
            dma((n,)),
            dma((n,)),
        ],
        compiler_params=pltpu.CompilerParams(
            collective_id=0, has_side_effects=True, vmem_limit_bytes=60 * 1024 * 1024
        ),
        name="attention_back",
    )(
        chosen,
        chosen,
        queries,
        keys.reshape(kblocks, KB, kv_cols),
        values.reshape(kblocks, KB, kv_cols),
        lse,
        out_grad,
        normed_input.T,
    )
    query_grad, key_grad, value_grad, weight_grad = outs
    return (
        query_grad,
        key_grad.reshape(tok, kv_cols),
        value_grad.reshape(tok, kv_cols),
        weight_grad,
    )


def solution(mesh):
    n, tp = mesh.shape["kv"], mesh.shape["tp"]
    in_specs = (P("kv", "tp"),) * 6 + (P("kv", None),)
    out_specs = (P("kv", "tp"),) * 4
    return jax.shard_map(
        functools.partial(local, n, tp),
        mesh=mesh,
        in_specs=in_specs,
        out_specs=out_specs,
        check_vma=False,
    )
```

```python
import functools

import jax
import jax.numpy as jnp
from jax import lax
from jax.experimental import pallas as pl
from jax.experimental.pallas import tpu as pltpu
from jax.sharding import PartitionSpec as P

HD = 128
QB = 64
KB = 32
NSEL = 16

MESH = pl.DeviceIdType.MESH
F32 = jnp.float32
BF16 = jnp.bfloat16


def remote(src, dst, send_sem, recv_sem, device_id):
    return pltpu.make_async_remote_copy(
        src_ref=src,
        dst_ref=dst,
        send_sem=send_sem,
        recv_sem=recv_sem,
        device_id=device_id,
        device_id_type=MESH,
    )


class Gather:
    def __init__(self, pool, send_z, send_x, send_c, recv, me, n, xs):
        self.pool, self.recv = pool, recv
        self.send_z, self.send_x, self.send_c = send_z, send_x, send_c
        self.me, self.n, self.xs = me, n, xs
        self.row = 2 * xs
        self.zs = n // self.row
        self.z = me // self.row
        self.r = me % self.row
        self.x = self.r // 2
        self.c = self.r % 2
        self.sends = self.zs - 1
        self.planes = self.zs

    def copy(self, slot, send_sem, dest):
        return remote(
            self.pool.at[slot], self.pool.at[slot], send_sem, self.recv.at[slot], {"kv": dest}
        )

    def plane(self, k):
        return (self.z - k + self.zs) % self.zs

    def along_z(self, k):
        dest = ((self.z + k) % self.zs) * self.row + self.r
        return self.copy(self.me, self.send_z.at[k], dest)

    def along_x(self, k, d):
        slot = self.plane(k) * self.row + self.r
        dest = self.z * self.row + ((self.x + d) % self.xs) * 2 + self.c
        return self.copy(slot, self.send_x.at[k, d], dest)

    def across(self, k, d):
        slot = self.plane(k) * self.row + ((self.x + d) % self.xs) * 2 + self.c
        dest = self.z * self.row + self.x * 2 + (1 - self.c)
        return self.copy(slot, self.send_c.at[k, d], dest)

    def wait_slot(self, slot):
        self.copy(slot, self.send_z.at[0], (self.me + 1) % self.n).wait_recv()

    def start(self):
        def body(k, _):
            self.along_z(k).start()
            return 0

        lax.fori_loop(1, self.sends + 1, body, 0)

    def relay(self):
        def step(k, first):
            slot = self.plane(k) * self.row + self.r
            if not first:
                self.wait_slot(slot)
            for d in range(1, self.xs):
                self.along_x(k, d).start()
            self.across(k, 0).start()

        def cross(k):
            for d in range(1, self.xs):
                slot = self.plane(k) * self.row + ((self.x + d) % self.xs) * 2 + self.c
                self.wait_slot(slot)
                self.across(k, d).start()

        step(0, True)

        def body(k, _):
            step(k, False)
            cross(k - 1)
            return 0

        lax.fori_loop(1, self.planes, body, 0)
        cross(self.planes - 1)

    def finish(self):
        def body(k, _):
            for d in range(self.xs):
                self.wait_slot(
                    self.plane(k) * self.row + ((self.x + d) % self.xs) * 2 + (1 - self.c)
                )
            return 0

        lax.fori_loop(0, self.planes, body, 0)

    def drain(self):
        def zbody(k, _):
            self.along_z(k).wait_send()
            return 0

        lax.fori_loop(1, self.sends + 1, zbody, 0)

        def body(k, _):
            for d in range(1, self.xs):
                self.along_x(k, d).wait_send()
            for d in range(self.xs):
                self.across(k, d).wait_send()
            return 0

        lax.fori_loop(0, self.planes, body, 0)


def dot(a, b, dims):
    return lax.dot_general(a, b, (dims, ((), ())), preferred_element_type=F32)


def kernel(
    n,
    tp,
    chosen,
    queries,
    keys,
    values,
    logsum,
    out_grad,
    normed,
    query_grad,
    key_grad,
    value_grad,
    weight_grad,
    pool,
    ask,
    asked,
    give,
    low_pool,
    norm_parts,
    norm_via,
    norm_pool,
    sel,
    s_buf,
    d_buf,
    p_low,
    ds_low,
    part,
    back,
    got,
    table,
    local_sem,
    ask_send,
    ask_recv,
    kv_send,
    kv_recv,
    back_send,
    back_recv,
    via_send,
    via_recv,
    norm_send,
    norm_recv,
    swap_send,
    swap_recv,
    lo_z,
    lo_x,
    lo_c,
    lo_recv,
):
    me = lax.axis_index("kv")
    col = lax.axis_index("tp")
    kblocks = keys.shape[0]
    tok = kblocks * KB
    qblocks = tok // QB
    kv_cols = keys.shape[2]
    kv_heads = kv_cols // HD
    group = queries.shape[1] // kv_cols
    per = n // tp
    sub = norm_parts.shape[2]
    rows = sub * tp
    scale = HD ** (-0.5)
    entries = qblocks * NSEL
    after = (me + 1) % n

    barrier = pltpu.get_barrier_semaphore()

    def greet(i, _):
        for t in range(tp):
            pl.semaphore_signal(
                barrier, inc=1, device_id={"kv": i, "tp": t}, device_id_type=MESH
            )
        return 0

    lax.fori_loop(0, n, greet, 0)
    own = []
    for w in range(kblocks):
        for a, ref in ((0, keys), (1, values)):
            c = pltpu.make_async_copy(ref.at[w], pool.at[n + w, a], local_sem.at[w, a])
            c.start()
            own.append(c)

    def look(i, _):
        block = jnp.int32(0)
        for b in range(qblocks):
            found = jnp.int32(entries)
            for e in range(NSEL):
                c = chosen[b, e]
                here = c // kblocks == i
                found = jnp.where(here, b * NSEL + e, found)
                block = jnp.where(here, c % kblocks + 1, block)
            table[b, i] = found
        ask[i] = jnp.full(ask.shape[1:], block, jnp.int32)
        return 0

    lax.fori_loop(0, me, look, 0)
    for m in range(normed.shape[1] // HD):
        turned = normed[:, m * HD : (m + 1) * HD].T
        for p in range(0, HD, sub):
            at = m * HD + p
            norm_parts[at % rows // sub, at // rows] = turned[p : p + sub]

    pl.semaphore_wait(barrier, n * tp)

    def ask_copy(i):
        return remote(ask.at[i], asked.at[me], ask_send.at[i], ask_recv.at[me], {"kv": i})

    def ask_start(i, _):
        ask_copy(i).start()
        return 0

    lax.fori_loop(0, me, ask_start, 0)

    def via_copy(d):
        q = (col + d) % tp
        return remote(
            norm_parts.at[q], norm_via.at[d], via_send.at[d], via_recv.at[d], {"tp": q}
        )

    for d in range(1, tp):
        via_copy(d).start()

    for w in range(kblocks):
        for b in range(qblocks):
            found = jnp.int32(entries)
            for e in range(NSEL):
                found = jnp.where(chosen[b, e] == me * kblocks + w, b * NSEL + e, found)
            table[b, n + w] = found
    part[:, entries] = jnp.zeros_like(part[:, entries])

    def kv_copy(j):
        return remote(give.at[j], pool.at[me], kv_send.at[j], kv_recv.at[me], {"kv": j})

    def answer(k, _):
        j = n - 1 - k
        remote(ask.at[0], asked.at[j], ask_send.at[0], ask_recv.at[j], {"kv": after}).wait_recv()
        named = asked[j]
        for a, ref in ((0, keys), (1, values)):
            block = jnp.zeros((KB, kv_cols), F32)
            for w in range(kblocks):
                mask = jnp.concatenate([named == w + 1] * (KB // 8), axis=0)
                block = jnp.where(mask, ref[w].astype(F32), block)
            give[j, a] = block.astype(BF16)
        kv_copy(j).start()
        return 0

    lax.fori_loop(0, n - 1 - me, answer, 0)

    def norm_each(act, act_local):
        def body(k0, _):
            for d in range(tp):
                t = (col + tp - d) % tp
                k = (k0 + me) % per
                dest = t * per + k
                src = norm_parts.at[col, k] if d == 0 else norm_via.at[d, k]

                @pl.when(dest == me)
                def _():
                    act_local(
                        pltpu.make_async_copy(src, norm_pool.at[col, me], norm_recv.at[me])
                    )

                @pl.when(dest != me)
                def _():
                    act(
                        remote(
                            src,
                            norm_pool.at[col, me],
                            norm_send.at[d, k],
                            norm_recv.at[me],
                            {"kv": dest},
                        )
                    )

            return 0

        lax.fori_loop(0, per, body, 0)

    for d in range(1, tp):
        via_copy(d).wait_recv()
    norm_each(lambda c: c.start(), lambda c: c.start())

    for c in own:
        c.wait()

    def kv_wait(j, _):
        remote(give.at[0], pool.at[j], kv_send.at[0], kv_recv.at[j], {"kv": after}).wait_recv()
        return 0

    lax.fori_loop(0, me, kv_wait, 0)
    span = NSEL * KB
    width = group * QB
    key_iota = lax.broadcasted_iota(jnp.int32, (KB, width), 0)
    row_iota = lax.broadcasted_iota(jnp.int32, (KB, width), 1) % QB
    logs = logsum[...].T
    for b in range(qblocks):
        for e in range(NSEL):
            block = chosen[b, e]
            owner = block // kblocks
            slot = jnp.where(owner == me, n + block % kblocks, jnp.where(owner < me, owner, n))
            for a in range(2):
                sel[a, e * KB : (e + 1) * KB, :] = pool[slot, a]
        for g in range(kv_heads):
            lanes = slice(g * HD, (g + 1) * HD)

            def stack(ref):
                return jnp.concatenate(
                    [
                        ref[b * QB : (b + 1) * QB, (g * group + h) * HD : (g * group + h + 1) * HD]
                        for h in range(group)
                    ],
                    axis=0,
                )

            q = stack(queries)
            do = stack(out_grad)
            k_sel = sel[0, :, lanes]
            s_buf[...] = dot(k_sel, q, ((1,), (1,)))
            d_buf[...] = dot(sel[1, :, lanes], do, ((1,), (1,)))
            log = jnp.concatenate(
                [
                    logs[g * group + h : g * group + h + 1, b * QB : (b + 1) * QB]
                    for h in range(group)
                ],
                axis=1,
            )
            delta = jnp.zeros((8, width), F32)
            for e in range(NSEL):
                at = slice(e * KB, (e + 1) * KB)
                limit = (me * tok + b * QB) - chosen[b, e] * KB
                valid = key_iota - row_iota <= limit
                p = jnp.where(valid, jnp.exp(s_buf[at, :] * scale - log), 0.0)
                s_buf[at, :] = p
                p_low[at, :] = p.astype(BF16)
                pd = p * d_buf[at, :]
                delta = delta + jnp.sum(pd.reshape(KB // 8, 8, width), axis=0)
            delta = jnp.sum(delta, axis=0, keepdims=True)
            for e in range(NSEL):
                at = slice(e * KB, (e + 1) * KB)
                ds_low[at, :] = (s_buf[at, :] * (d_buf[at, :] - delta)).astype(BF16)
            ds = ds_low[...]
            here = slice(b * NSEL, (b + 1) * NSEL)
            part[0, here, :, lanes] = (dot(ds, q, ((1,), (0,))) * scale).reshape(NSEL, KB, HD)
            part[1, here, :, lanes] = dot(p_low[...], do, ((1,), (0,))).reshape(NSEL, KB, HD)
            dq = dot(ds, k_sel, ((0,), (0,))) * scale
            for h in range(group):
                query_grad[
                    b * QB : (b + 1) * QB, (g * group + h) * HD : (g * group + h + 1) * HD
                ] = dq[h * QB : (h + 1) * QB]

    def back_copy(i):
        return remote(back.at[i], got.at[me], back_send.at[i], back_recv.at[me], {"kv": i})

    def send_back(i, _):
        for a in range(2):
            total = part[a, table[0, i]]
            for b in range(1, qblocks):
                total = total + part[a, table[b, i]]
            back[i, a] = total.astype(BF16)
        back_copy(i).start()
        return 0

    lax.fori_loop(0, me, send_back, 0)

    for w in range(kblocks):
        for a, out in ((0, key_grad), (1, value_grad)):
            total = part[a, table[0, n + w]]
            for b in range(1, qblocks):
                total = total + part[a, table[b, n + w]]
            out[w] = total

    def swap_copy(d):
        q = (col + d) % tp
        return remote(
            norm_pool.at[col], norm_pool.at[col], swap_send.at[d], swap_recv.at[d], {"tp": q}
        )

    def norm_wait(j, _):
        pltpu.make_async_copy(
            norm_pool.at[col, j], norm_pool.at[col, j], norm_recv.at[j]
        ).wait()
        return 0

    lax.fori_loop(0, n, norm_wait, 0)
    for d in range(1, tp):
        swap_copy(d).start()

    def add_back(j, _):
        remote(
            back.at[0], got.at[j], back_send.at[0], back_recv.at[j], {"kv": after}
        ).wait_recv()
        named = asked[j]
        terms = [got[j, a].astype(F32) for a in range(2)]
        for w in range(kblocks):
            mask = jnp.concatenate([named == w + 1] * (KB // 8), axis=0)
            for a, out in ((0, key_grad), (1, value_grad)):
                out[w] += jnp.where(mask, terms[a], 0.0)
        return 0

    lax.fori_loop(me + 1, n, add_back, 0)

    low_pool[me] = value_grad[...].reshape(tok, kv_cols).astype(BF16)
    low = Gather(low_pool, lo_z, lo_x, lo_c, lo_recv, me, n, tp)
    low.start()
    low.relay()
    for d in range(1, tp):
        q = (col + tp - d) % tp
        remote(
            norm_pool.at[q], norm_pool.at[q], swap_send.at[d], swap_recv.at[d], {"tp": q}
        ).wait_recv()
    low.finish()

    row = low.row

    def product(z, q):
        a = jnp.concatenate([norm_pool[q, z * row + i] for i in range(row)], axis=1)
        v = jnp.concatenate([low_pool[z * row + i] for i in range(row)], axis=0)
        return dot(a, v, ((1,), (0,)))

    for q in range(tp):
        weight_grad[q * sub : (q + 1) * sub] = product(0, q)

    def weigh(z, _):
        for q in range(tp):
            weight_grad[q * sub : (q + 1) * sub] += product(z, q)
        return 0

    lax.fori_loop(1, low.zs, weigh, 0)

    low.drain()

    def drain_early(i, _):
        ask_copy(i).wait_send()
        back_copy(i).wait_send()
        return 0

    lax.fori_loop(0, me, drain_early, 0)

    def drain_late(j, _):
        kv_copy(j).wait_send()
        return 0

    lax.fori_loop(me + 1, n, drain_late, 0)
    for d in range(1, tp):
        via_copy(d).wait_send()
        swap_copy(d).wait_send()
    norm_each(lambda c: c.wait_send(), lambda c: None)


def local(n, tp, queries, keys, values, logsum, out_grad, normed_input, chosen):
    tok, kv_cols = keys.shape
    kv_heads = kv_cols // HD
    group = queries.shape[1] // kv_cols
    kblocks = tok // KB
    qblocks = tok // QB
    rows = normed_input.shape[1] * tp // n
    zs = n // (2 * tp)
    entries = qblocks * NSEL
    span = NSEL * KB
    width = group * QB
    per = n // tp
    vmem = pl.BlockSpec(memory_space=pltpu.VMEM)
    dma = pltpu.SemaphoreType.DMA
    outs = pl.pallas_call(
        functools.partial(kernel, n, tp),
        out_shape=(
            jax.ShapeDtypeStruct((tok, queries.shape[1]), F32),
            jax.ShapeDtypeStruct((kblocks, KB, kv_cols), F32),
            jax.ShapeDtypeStruct((kblocks, KB, kv_cols), F32),
            jax.ShapeDtypeStruct((rows, kv_cols), F32),
        ),
        in_specs=[pl.BlockSpec(memory_space=pltpu.SMEM)] + [vmem] * 6,
        out_specs=(vmem,) * 4,
        scratch_shapes=[
            pltpu.VMEM((n + kblocks, 2, KB, kv_cols), BF16),
            pltpu.VMEM((n, 8, kv_cols), jnp.int32),
            pltpu.VMEM((n, 8, kv_cols), jnp.int32),
            pltpu.VMEM((n, 2, KB, kv_cols), BF16),
            pltpu.VMEM((n, tok, kv_cols), BF16),
            pltpu.VMEM((tp, per, rows // tp, tok), BF16),
            pltpu.VMEM((tp, per, rows // tp, tok), BF16),
            pltpu.VMEM((tp, n, rows // tp, tok), BF16),
            pltpu.VMEM((2, span, kv_cols), BF16),
            pltpu.VMEM((span, width), F32),
            pltpu.VMEM((span, width), F32),
            pltpu.VMEM((span, width), BF16),
            pltpu.VMEM((span, width), BF16),
            pltpu.VMEM((2, entries + 1, KB, kv_cols), F32),
            pltpu.VMEM((n, 2, KB, kv_cols), BF16),
            pltpu.VMEM((n, 2, KB, kv_cols), BF16),
            pltpu.SMEM((qblocks, n + kblocks), jnp.int32),
            dma((kblocks, 2)),
            dma((n,)),
            dma((n,)),
            dma((n,)),
            dma((n,)),
            dma((n,)),
            dma((n,)),
            dma((tp,)),
            dma((tp,)),
            dma((tp, per)),
            dma((n,)),
            dma((tp,)),
            dma((tp,)),
            dma((zs,)),
            dma((zs, tp)),
            dma((zs, tp)),
            dma((n,)),
        ],
        compiler_params=pltpu.CompilerParams(
            collective_id=0, has_side_effects=True, vmem_limit_bytes=60 * 1024 * 1024
        ),
        name="attention_back",
    )(
        chosen,
        queries,
        keys.reshape(kblocks, KB, kv_cols),
        values.reshape(kblocks, KB, kv_cols),
        logsum,
        out_grad,
        normed_input,
    )
    query_grad, key_grad, value_grad, weight_grad = outs
    return (
        query_grad,
        key_grad.reshape(tok, kv_cols),
        value_grad.reshape(tok, kv_cols),
        weight_grad,
    )


def solution(mesh):
    n, tp = mesh.shape["kv"], mesh.shape["tp"]
    in_specs = (P("kv", "tp"),) * 6 + (P("kv", None),)
    out_specs = (P("kv", "tp"),) * 4
    return jax.shard_map(
        functools.partial(local, n, tp),
        mesh=mesh,
        in_specs=in_specs,
        out_specs=out_specs,
        check_vma=False,
    )
```

```python
import functools

import jax
import jax.numpy as jnp
from jax import lax
from jax.experimental import pallas as pl
from jax.experimental.pallas import tpu as pltpu
from jax.sharding import PartitionSpec as P

HD = 128
QB = 64
KB = 32
NSEL = 16

MESH = pl.DeviceIdType.MESH
F32 = jnp.float32
BF16 = jnp.bfloat16


def remote(src, dst, send_sem, recv_sem, device_id):
    return pltpu.make_async_remote_copy(
        src_ref=src,
        dst_ref=dst,
        send_sem=send_sem,
        recv_sem=recv_sem,
        device_id=device_id,
        device_id_type=MESH,
    )


class Gather:
    def __init__(self, pool, send_z, send_x, send_c, recv, me, n, xs):
        self.pool, self.recv = pool, recv
        self.send_z, self.send_x, self.send_c = send_z, send_x, send_c
        self.me, self.n, self.xs = me, n, xs
        self.row = 2 * xs
        self.zs = n // self.row
        self.z = me // self.row
        self.r = me % self.row
        self.x = self.r // 2
        self.c = self.r % 2
        self.sends = self.zs - 1
        self.planes = self.zs

    def copy(self, slot, send_sem, dest):
        return remote(
            self.pool.at[slot], self.pool.at[slot], send_sem, self.recv.at[slot], {"kv": dest}
        )

    def plane(self, k):
        return (self.z - k + self.zs) % self.zs

    def along_z(self, k):
        dest = ((self.z + k) % self.zs) * self.row + self.r
        return self.copy(self.me, self.send_z.at[k], dest)

    def along_x(self, k, d):
        slot = self.plane(k) * self.row + self.r
        dest = self.z * self.row + ((self.x + d) % self.xs) * 2 + self.c
        return self.copy(slot, self.send_x.at[k, d], dest)

    def across(self, k, d):
        slot = self.plane(k) * self.row + ((self.x + d) % self.xs) * 2 + self.c
        dest = self.z * self.row + self.x * 2 + (1 - self.c)
        return self.copy(slot, self.send_c.at[k, d], dest)

    def wait_slot(self, slot):
        self.copy(slot, self.send_z.at[0], (self.me + 1) % self.n).wait_recv()

    def start(self):
        def body(k, _):
            self.along_z(k).start()
            return 0

        lax.fori_loop(1, self.sends + 1, body, 0)

    def relay(self):
        def step(k, first):
            slot = self.plane(k) * self.row + self.r
            if not first:
                self.wait_slot(slot)
            for d in range(1, self.xs):
                self.along_x(k, d).start()
            self.across(k, 0).start()

        def cross(k):
            for d in range(1, self.xs):
                slot = self.plane(k) * self.row + ((self.x + d) % self.xs) * 2 + self.c
                self.wait_slot(slot)
                self.across(k, d).start()

        step(0, True)

        def body(k, _):
            step(k, False)
            cross(k - 1)
            return 0

        lax.fori_loop(1, self.planes, body, 0)
        cross(self.planes - 1)

    def finish(self):
        def body(k, _):
            for d in range(self.xs):
                self.wait_slot(
                    self.plane(k) * self.row + ((self.x + d) % self.xs) * 2 + (1 - self.c)
                )
            return 0

        lax.fori_loop(0, self.planes, body, 0)

    def drain(self):
        def zbody(k, _):
            self.along_z(k).wait_send()
            return 0

        lax.fori_loop(1, self.sends + 1, zbody, 0)

        def body(k, _):
            for d in range(1, self.xs):
                self.along_x(k, d).wait_send()
            for d in range(self.xs):
                self.across(k, d).wait_send()
            return 0

        lax.fori_loop(0, self.planes, body, 0)


def dot(a, b, dims):
    return lax.dot_general(a, b, (dims, ((), ())), preferred_element_type=F32)


def kernel(
    n,
    tp,
    chosen,
    queries,
    keys,
    values,
    logsum,
    out_grad,
    normed,
    query_grad,
    key_grad,
    value_grad,
    weight_grad,
    ask,
    asked,
    give,
    low_pool,
    norm_parts,
    norm_via,
    norm_pool,
    sel,
    s_buf,
    d_buf,
    p_low,
    ds_low,
    part,
    back,
    got,
    table,
    local_sem,
    ask_send,
    ask_recv,
    kv_send,
    kv_recv,
    back_send,
    back_recv,
    via_send,
    via_recv,
    norm_send,
    norm_recv,
    swap_send,
    swap_recv,
    lo_z,
    lo_x,
    lo_c,
    lo_recv,
    *pools,
):
    me = lax.axis_index("kv")
    col = lax.axis_index("tp")
    kblocks = keys.shape[0]
    tok = kblocks * KB
    qblocks = tok // QB
    kv_cols = keys.shape[2]
    kv_heads = kv_cols // HD
    group = queries.shape[1] // kv_cols
    per = n // tp
    sub = norm_parts.shape[2]
    rows = sub * tp
    scale = HD ** (-0.5)
    entries = qblocks * NSEL
    after = (me + 1) % n

    barrier = pltpu.get_barrier_semaphore()

    def greet(i, _):
        for t in range(tp):
            pl.semaphore_signal(
                barrier, inc=1, device_id={"kv": i, "tp": t}, device_id_type=MESH
            )
        return 0

    lax.fori_loop(0, n, greet, 0)
    own = []
    for w in range(kblocks):
        for a, ref in ((0, keys), (1, values)):
            for g in range(kv_heads):
                c = pltpu.make_async_copy(
                    ref.at[w, :, g * HD : (g + 1) * HD],
                    pools[g].at[n + w, a],
                    local_sem.at[g, w, a],
                )
                c.start()
                own.append(c)

    def look(i, _):
        block = jnp.int32(0)
        for b in range(qblocks):
            found = jnp.int32(entries)
            for e in range(NSEL):
                c = chosen[b, e]
                here = c // kblocks == i
                found = jnp.where(here, b * NSEL + e, found)
                block = jnp.where(here, c % kblocks + 1, block)
            table[b, i] = found
        ask[i] = jnp.full(ask.shape[1:], block, jnp.int32)
        return 0

    lax.fori_loop(0, me, look, 0)
    for m in range(normed.shape[1] // HD):
        turned = normed[:, m * HD : (m + 1) * HD].T
        for p in range(0, HD, sub):
            at = m * HD + p
            norm_parts[at % rows // sub, at // rows] = turned[p : p + sub]

    pl.semaphore_wait(barrier, n * tp)

    def ask_copy(i):
        return remote(ask.at[i], asked.at[me], ask_send.at[i], ask_recv.at[me], {"kv": i})

    def ask_start(i, _):
        ask_copy(i).start()
        return 0

    lax.fori_loop(0, me, ask_start, 0)

    def via_copy(d):
        q = (col + d) % tp
        return remote(
            norm_parts.at[q], norm_via.at[d], via_send.at[d], via_recv.at[d], {"tp": q}
        )

    for d in range(1, tp):
        via_copy(d).start()

    for w in range(kblocks):
        for b in range(qblocks):
            found = jnp.int32(entries)
            for e in range(NSEL):
                found = jnp.where(chosen[b, e] == me * kblocks + w, b * NSEL + e, found)
            table[b, n + w] = found
    part[:, :, entries] = jnp.zeros_like(part[:, :, entries])

    def kv_copy(g, j):
        return remote(
            give.at[g, j], pools[g].at[me], kv_send.at[g, j], kv_recv.at[g, me], {"kv": j}
        )

    def answer(g):
        lanes = slice(g * HD, (g + 1) * HD)

        def body(k, _):
            j = n - 1 - k
            if g == 0:
                remote(
                    ask.at[0], asked.at[j], ask_send.at[0], ask_recv.at[j], {"kv": after}
                ).wait_recv()
            named = asked[j]
            for a, ref in ((0, keys), (1, values)):
                block = jnp.zeros((KB, HD), F32)
                for w in range(kblocks):
                    mask = jnp.concatenate([named == w + 1] * (KB // 8), axis=0)
                    block = jnp.where(mask, ref[w, :, lanes].astype(F32), block)
                give[g, j, a] = block.astype(BF16)
            kv_copy(g, j).start()
            return 0

        lax.fori_loop(0, n - 1 - me, body, 0)

    def norm_each(act, act_local, ds, lower, upper):
        def body(k0, _):
            for d in ds:
                t = (col + tp - d) % tp
                k = (k0 + me) % per
                dest = t * per + k
                src = norm_parts.at[col, k] if d == 0 else norm_via.at[d, k]

                @pl.when((dest == me) & upper)
                def _():
                    act_local(
                        pltpu.make_async_copy(src, norm_pool.at[col, me], norm_recv.at[me])
                    )

                @pl.when(((dest < me) & lower) | ((dest > me) & upper))
                def _():
                    act(
                        remote(
                            src,
                            norm_pool.at[col, me],
                            norm_send.at[d, k],
                            norm_recv.at[me],
                            {"kv": dest},
                        )
                    )

            return 0

        lax.fori_loop(0, per, body, 0)

    def begin(c):
        c.start()

    norm_each(begin, begin, (0,), True, False)
    for g in range(kv_heads):
        answer(g)
    for d in range(1, tp):
        via_copy(d).wait_recv()
    norm_each(begin, begin, range(1, tp), True, False)
    norm_each(begin, begin, range(1, tp), False, True)
    norm_each(begin, begin, (0,), False, True)

    for c in own:
        c.wait()

    span = NSEL * KB
    width = group * QB
    key_iota = lax.broadcasted_iota(jnp.int32, (KB, width), 0)
    row_iota = lax.broadcasted_iota(jnp.int32, (KB, width), 1) % QB
    logs = logsum[...].T

    def back_copy(g, i):
        return remote(
            back.at[g, i], got.at[g, me], back_send.at[g, i], back_recv.at[g, me], {"kv": i}
        )

    for g in range(kv_heads):
        lanes = slice(g * HD, (g + 1) * HD)

        def kv_wait(j, _):
            remote(
                give.at[g, 0], pools[g].at[j], kv_send.at[g, 0], kv_recv.at[g, j], {"kv": after}
            ).wait_recv()
            return 0

        lax.fori_loop(0, me, kv_wait, 0)
        for b in range(qblocks):
            for e in range(NSEL):
                block = chosen[b, e]
                owner = block // kblocks
                slot = jnp.where(owner == me, n + block % kblocks, jnp.where(owner < me, owner, n))
                for a in range(2):
                    sel[a, e * KB : (e + 1) * KB] = pools[g][slot, a]

            def stack(ref):
                return jnp.concatenate(
                    [
                        ref[b * QB : (b + 1) * QB, (g * group + h) * HD : (g * group + h + 1) * HD]
                        for h in range(group)
                    ],
                    axis=0,
                )

            q = stack(queries)
            do = stack(out_grad)
            k_sel = sel[0]
            s_buf[...] = dot(k_sel, q, ((1,), (1,)))
            d_buf[...] = dot(sel[1], do, ((1,), (1,)))
            log = jnp.concatenate(
                [
                    logs[g * group + h : g * group + h + 1, b * QB : (b + 1) * QB]
                    for h in range(group)
                ],
                axis=1,
            )
            delta = jnp.zeros((8, width), F32)
            for e in range(NSEL):
                at = slice(e * KB, (e + 1) * KB)
                limit = (me * tok + b * QB) - chosen[b, e] * KB
                valid = key_iota - row_iota <= limit
                p = jnp.where(valid, jnp.exp(s_buf[at, :] * scale - log), 0.0)
                s_buf[at, :] = p
                p_low[at, :] = p.astype(BF16)
                pd = p * d_buf[at, :]
                delta = delta + jnp.sum(pd.reshape(KB // 8, 8, width), axis=0)
            delta = jnp.sum(delta, axis=0, keepdims=True)
            for e in range(NSEL):
                at = slice(e * KB, (e + 1) * KB)
                ds_low[at, :] = (s_buf[at, :] * (d_buf[at, :] - delta)).astype(BF16)
            ds = ds_low[...]
            here = slice(b * NSEL, (b + 1) * NSEL)
            part[g, 0, here] = (dot(ds, q, ((1,), (0,))) * scale).reshape(NSEL, KB, HD)
            part[g, 1, here] = dot(p_low[...], do, ((1,), (0,))).reshape(NSEL, KB, HD)
            dq = dot(ds, k_sel, ((0,), (0,))) * scale
            for h in range(group):
                query_grad[
                    b * QB : (b + 1) * QB, (g * group + h) * HD : (g * group + h + 1) * HD
                ] = dq[h * QB : (h + 1) * QB]

        def send_back(i, _):
            for a in range(2):
                total = part[g, a, table[0, i]]
                for b in range(1, qblocks):
                    total = total + part[g, a, table[b, i]]
                back[g, i, a] = total.astype(BF16)
            back_copy(g, i).start()
            return 0

        lax.fori_loop(0, me, send_back, 0)

    for w in range(kblocks):
        for g in range(kv_heads):
            for a, out in ((0, key_grad), (1, value_grad)):
                total = part[g, a, table[0, n + w]]
                for b in range(1, qblocks):
                    total = total + part[g, a, table[b, n + w]]
                out[w, :, g * HD : (g + 1) * HD] = total

    def swap_copy(d):
        q = (col + d) % tp
        return remote(
            norm_pool.at[col], norm_pool.at[col], swap_send.at[d], swap_recv.at[d], {"tp": q}
        )

    def norm_wait(j, _):
        pltpu.make_async_copy(
            norm_pool.at[col, j], norm_pool.at[col, j], norm_recv.at[j]
        ).wait()
        return 0

    lows = [
        Gather(low_pool.at[g], lo_z.at[g], lo_x.at[g], lo_c.at[g], lo_recv.at[g], me, n, tp)
        for g in range(kv_heads)
    ]

    for g in range(kv_heads):
        lanes = slice(g * HD, (g + 1) * HD)

        def add_back(j, _):
            remote(
                back.at[g, 0], got.at[g, j], back_send.at[g, 0], back_recv.at[g, j], {"kv": after}
            ).wait_recv()
            named = asked[j]
            terms = [got[g, j, a].astype(F32) for a in range(2)]
            for w in range(kblocks):
                mask = jnp.concatenate([named == w + 1] * (KB // 8), axis=0)
                for a, out in ((0, key_grad), (1, value_grad)):
                    out[w, :, lanes] += jnp.where(mask, terms[a], 0.0)
            return 0

        lax.fori_loop(me + 1, n, add_back, 0)
        low_pool[g, me] = value_grad[:, :, lanes].reshape(tok, HD).astype(BF16)
        lows[g].start()
        if g == 0:
            lax.fori_loop(0, n, norm_wait, 0)
            for d in range(1, tp):
                swap_copy(d).start()

    for low in lows:
        low.relay()
    for d in range(1, tp):
        q = (col + tp - d) % tp
        remote(
            norm_pool.at[q], norm_pool.at[q], swap_send.at[d], swap_recv.at[d], {"tp": q}
        ).wait_recv()
    row, zs = lows[0].row, lows[0].zs
    for g in range(kv_heads):
        lanes = slice(g * HD, (g + 1) * HD)
        lows[g].finish()

        def product(z, q):
            a = jnp.concatenate([norm_pool[q, z * row + i] for i in range(row)], axis=1)
            v = jnp.concatenate([low_pool[g, z * row + i] for i in range(row)], axis=0)
            return dot(a, v, ((1,), (0,)))

        for q in range(tp):
            weight_grad[q * sub : (q + 1) * sub, lanes] = product(0, q)

        def weigh(z, _):
            for q in range(tp):
                weight_grad[q * sub : (q + 1) * sub, lanes] += product(z, q)
            return 0

        lax.fori_loop(1, zs, weigh, 0)

    for low in lows:
        low.drain()

    def drain_early(i, _):
        ask_copy(i).wait_send()
        for g in range(kv_heads):
            back_copy(g, i).wait_send()
        return 0

    lax.fori_loop(0, me, drain_early, 0)

    def drain_late(j, _):
        for g in range(kv_heads):
            kv_copy(g, j).wait_send()
        return 0

    lax.fori_loop(me + 1, n, drain_late, 0)
    for d in range(1, tp):
        via_copy(d).wait_send()
        swap_copy(d).wait_send()
    norm_each(lambda c: c.wait_send(), lambda c: None, range(tp), True, True)


def local(n, tp, queries, keys, values, logsum, out_grad, normed_input, chosen):
    tok, kv_cols = keys.shape
    kv_heads = kv_cols // HD
    group = queries.shape[1] // kv_cols
    kblocks = tok // KB
    qblocks = tok // QB
    rows = normed_input.shape[1] * tp // n
    zs = n // (2 * tp)
    entries = qblocks * NSEL
    span = NSEL * KB
    width = group * QB
    per = n // tp
    vmem = pl.BlockSpec(memory_space=pltpu.VMEM)
    dma = pltpu.SemaphoreType.DMA
    outs = pl.pallas_call(
        functools.partial(kernel, n, tp),
        out_shape=(
            jax.ShapeDtypeStruct((tok, queries.shape[1]), F32),
            jax.ShapeDtypeStruct((kblocks, KB, kv_cols), F32),
            jax.ShapeDtypeStruct((kblocks, KB, kv_cols), F32),
            jax.ShapeDtypeStruct((rows, kv_cols), F32),
        ),
        in_specs=[pl.BlockSpec(memory_space=pltpu.SMEM)] + [vmem] * 6,
        out_specs=(vmem,) * 4,
        scratch_shapes=[
            pltpu.VMEM((n, 8, HD), jnp.int32),
            pltpu.VMEM((n, 8, HD), jnp.int32),
            pltpu.VMEM((kv_heads, n, 2, KB, HD), BF16),
            pltpu.VMEM((kv_heads, n, tok, HD), BF16),
            pltpu.VMEM((tp, per, rows // tp, tok), BF16),
            pltpu.VMEM((tp, per, rows // tp, tok), BF16),
            pltpu.VMEM((tp, n, rows // tp, tok), BF16),
            pltpu.VMEM((2, span, HD), BF16),
            pltpu.VMEM((span, width), F32),
            pltpu.VMEM((span, width), F32),
            pltpu.VMEM((span, width), BF16),
            pltpu.VMEM((span, width), BF16),
            pltpu.VMEM((kv_heads, 2, entries + 1, KB, HD), F32),
            pltpu.VMEM((kv_heads, n, 2, KB, HD), BF16),
            pltpu.VMEM((kv_heads, n, 2, KB, HD), BF16),
            pltpu.SMEM((qblocks, n + kblocks), jnp.int32),
            dma((kv_heads, kblocks, 2)),
            dma((n,)),
            dma((n,)),
            dma((kv_heads, n)),
            dma((kv_heads, n)),
            dma((kv_heads, n)),
            dma((kv_heads, n)),
            dma((tp,)),
            dma((tp,)),
            dma((tp, per)),
            dma((n,)),
            dma((tp,)),
            dma((tp,)),
            dma((kv_heads, zs)),
            dma((kv_heads, zs, tp)),
            dma((kv_heads, zs, tp)),
            dma((kv_heads, n)),
        ]
        + [pltpu.VMEM((n + kblocks, 2, KB, HD), BF16)] * kv_heads,
        compiler_params=pltpu.CompilerParams(
            collective_id=0, has_side_effects=True, vmem_limit_bytes=60 * 1024 * 1024
        ),
        name="attention_back",
    )(
        chosen,
        queries,
        keys.reshape(kblocks, KB, kv_cols),
        values.reshape(kblocks, KB, kv_cols),
        logsum,
        out_grad,
        normed_input,
    )
    query_grad, key_grad, value_grad, weight_grad = outs
    return (
        query_grad,
        key_grad.reshape(tok, kv_cols),
        value_grad.reshape(tok, kv_cols),
        weight_grad,
    )


def solution(mesh):
    n, tp = mesh.shape["kv"], mesh.shape["tp"]
    in_specs = (P("kv", "tp"),) * 6 + (P("kv", None),)
    out_specs = (P("kv", "tp"),) * 4
    return jax.shard_map(
        functools.partial(local, n, tp),
        mesh=mesh,
        in_specs=in_specs,
        out_specs=out_specs,
        check_vma=False,
    )
```
